32 devices in a mesh: sp: 8 (over z, x), dp: 4 (over y, core).
Axes of the slice: x: 2, y: 2, z: 4, core: 2. Of those that a mesh axis runs over, the one named last changes fastest.
Arguments:
- queries: bfloat16 [4, 1024, 2048], P('dp', 'sp'), may hold values from -9 to 9
- keys: bfloat16 [4, 1024, 512], P('dp', 'sp'), may hold values from -9 to 9
- values: bfloat16 [4, 1024, 512], P('dp', 'sp'), may hold values from -6 to 6
- out_grad: bfloat16 [4, 1024, 2048], P('dp', 'sp'), may hold values from -24 to 24
- layer_in: bfloat16 [4, 1024, 4096], P('dp', 'sp'), may hold values from -0.1875 to 0.1875
- key_weight: bfloat16 [4096, 512], P('dp'), may hold values from -0.09375 to 0.09375
- value_weight: bfloat16 [4096, 512], P('dp'), may hold values from -0.09375 to 0.09375
- query_gain: float32 [128], replicated, may hold values from 0.64 to 6.04
- key_gain: float32 [128], replicated, may hold values from 0.64 to 6.04
Outputs:
- grad_query: bfloat16 [4, 1024, 2048], P('dp', 'sp')
- grad_in: bfloat16 [4, 1024, 4096], P('dp', 'sp')
- grad_key_weight: float32 [4096, 512], P('dp')
- grad_value_weight: float32 [4096, 512], P('dp')
The draws below stay inside these ranges and needn't reach their ends.
All inputs are finite; a program needn't handle non-finite values.
Results may differ from the reference program's by a relative error of at most 0.018.
The reference program's roundings to bfloat16 on the way count: a program that leaves them out, or rounds other values in their place, can miss the bound.
Values may be sent and summed in bfloat16 or wider, within the bound.
A program may use at most 128 MiB of HBM per device.

```python
import math
from functools import partial
import jax
import jax.numpy as jnp
from jax import lax

D = 4096
HEADS = 16
KV_HEADS = 4
HEAD_DIM = 128
GRID_W = 64
TOK_DEV = 128
LEN = 1024
SEQS = 4
QW = 2048
KVW = 512
N_SP = 8
N_DP = 4


def gain_values(key, salt):
    base = jax.random.uniform(jax.random.fold_in(key, salt), (HEAD_DIM,), jnp.float32)
    return 0.64 + 0.72 * base


def draw_query_gain(key, part):
    return gain_values(key, 101)


def draw_key_gain(key, part):
    return gain_values(key, 102)


def drawn(key):
    seq_count = N_DP
    length = TOK_DEV * N_SP
    key_base = jnp.clip(jax.random.normal(jax.random.fold_in(key, 11), (seq_count, length, KV_HEADS * HEAD_DIM), jnp.float32), -6.0, 6.0)
    query_base = jnp.clip(jax.random.normal(jax.random.fold_in(key, 12), (seq_count, length, HEADS * HEAD_DIM), jnp.float32), -6.0, 6.0)
    return (jnp.clip(query_base, -9.0, 9.0), jnp.clip(key_base, -9.0, 9.0))


def draw_queries(key, part):
    return drawn(key)[0].astype(jnp.bfloat16)


def draw_keys(key, part):
    return drawn(key)[1].astype(jnp.bfloat16)


def spiked(entries, own_key, source, target, shards_of, factor):
    def block_of(dim):
        return (jnp.arange(entries.shape[dim]) // (entries.shape[dim] // shards_of)).reshape((-1,) + (1,) * (entries.ndim - 1 - dim))

    one_side = jax.random.permutation(own_key, shards_of)[block_of(target)]
    far = (block_of(target) + shards_of // 2) % shards_of
    return jnp.where((block_of(source) == one_side) | (block_of(source) == far), factor * entries, entries)


def level_of(own_key, extent, cuts, least, top_value):
    def one(dim, parts):
        heights = jax.random.uniform(jax.random.fold_in(jax.random.fold_in(own_key, 6), dim), (parts,), jnp.float32, least / len(cuts), top_value / len(cuts))
        return jnp.repeat(jnp.exp(heights), extent[dim] // parts).reshape((-1,) + (1,) * (len(extent) - dim - 1))

    loudness = one(*cuts[0])
    for cut in cuts[1:]:
        loudness = loudness * one(*cut)
    return loudness


def scatter_about(stream_key, dims, scale, reach, cuts=(), kind=jnp.bfloat16):
    values = jax.random.normal(stream_key, dims, jnp.float32) * scale
    if len(cuts) > 0:
        values = level_of(stream_key, dims, cuts, -0.22, 0.18) * values
    return jnp.clip(values, min=-reach, max=reach).astype(kind)


def heavy_noise(own_key, dims, width, most, cuts, heavy, kind=jnp.bfloat16):
    drawn = width * jax.random.normal(own_key, dims, jnp.float32)
    if cuts:
        drawn = drawn * level_of(own_key, dims, cuts, -0.22, 0.18)
    return jnp.clip(spiked(drawn, jax.random.fold_in(own_key, 3), *heavy), -most, most).astype(kind)


def setup_inputs(seed: int = 0) -> dict:
    key_of = jax.random.split(jax.random.key(seed), 10)
    return {
        "queries": draw_queries(jax.random.fold_in(key_of[9], 71), 0),
        "keys": draw_keys(jax.random.fold_in(key_of[9], 71), 0),
        "values": scatter_about(key_of[2], (SEQS, LEN, KVW), 1.0, 6.0, ((0, 4), (1, 8))),
        "out_grad": scatter_about(key_of[3], (SEQS, LEN, QW), 4.0, 24.0, ((0, 4), (1, 8))),
        "layer_in": heavy_noise(key_of[4], (SEQS, LEN, D), (2.0 / (N_DP * N_SP * TOK_DEV) ** 0.5), 0.1875, ((0, 4), (1, 8)), (1, 2, 8, 2.0)),
        "key_weight": scatter_about(key_of[5], (D, KVW), D ** -0.5, 0.09375, ((0, 4),)),
        "value_weight": scatter_about(key_of[6], (D, KVW), D ** -0.5, 0.09375, ((0, 4),)),
        "query_gain": draw_query_gain(jax.random.fold_in(key_of[9], 71), 0),
        "key_gain": draw_key_gain(jax.random.fold_in(key_of[9], 71), 0),
    }


epsilon = 1e-06
rope_base = 10000.0

def norm_rotate(vector, gain_vec, row_index, col_index):
    scaled = vector * lax.rsqrt(lax.optimization_barrier(jnp.mean(vector * vector, axis=-1, keepdims=True)) + epsilon) * gain_vec
    quarter = vector.shape[-1] // 4
    inverse = rope_base ** (-jnp.arange(quarter, dtype=jnp.float32) / quarter)
    pieces = []
    for offset, position in ((0, row_index), (2 * quarter, col_index)):
        angles = position.astype(jnp.float32)[:, None] * inverse[None, :]
        cosine = jnp.cos(angles)
        sine_part = jnp.sin(angles)
        first_half = scaled[:, offset:offset + quarter]
        second_half = scaled[:, offset + quarter:offset + 2 * quarter]
        pieces.append(first_half * cosine - second_half * sine_part)
        pieces.append(first_half * sine_part + second_half * cosine)
    return jnp.concatenate(pieces, axis=1)

def contract_cols(left_side, right_side):
    return lax.dot_general(left_side, right_side, (((1,), (1,)), ((), ())), preferred_element_type=jnp.float32)

def contract_rows(left_side, right_side):
    return lax.dot_general(left_side, right_side, (((0,), (0,)), ((), ())), preferred_element_type=jnp.float32)

def head_grads(query_rows, grad_rows, key_rows, value_rows, query_gain, key_gain):
    length = query_rows.shape[0]
    block_rows = math.gcd(length, 512)
    positions = jnp.arange(length, dtype=jnp.int32)
    row_index = positions // GRID_W
    col_index = positions % GRID_W
    q_rot, q_back = jax.vjp(partial(norm_rotate, gain_vec=query_gain, row_index=row_index, col_index=col_index), query_rows.astype(jnp.float32))
    k_rot, k_back = jax.vjp(partial(norm_rotate, gain_vec=key_gain, row_index=row_index, col_index=col_index), key_rows.astype(jnp.float32))
    q_bf = q_rot.astype(jnp.bfloat16)
    k_bf = k_rot.astype(jnp.bfloat16)
    score_scale = q_rot.shape[-1] ** (-0.5)

    def one_block(accums, block_index):
        k_acc, v_acc = accums
        row_start = block_index * block_rows
        q_block = lax.dynamic_slice_in_dim(q_bf, row_start, block_rows, 0)
        g_block = lax.dynamic_slice_in_dim(grad_rows, row_start, block_rows, 0)
        scores = contract_cols(q_block, k_bf) * score_scale
        shifted = jnp.exp(scores - lax.optimization_barrier(jnp.max(scores, axis=1, keepdims=True)))
        attn_probs = shifted / lax.optimization_barrier(jnp.sum(shifted, axis=1, keepdims=True))
        probs_b = attn_probs.astype(jnp.bfloat16)
        attn_out = jnp.dot(probs_b, value_rows, preferred_element_type=jnp.float32)
        row_delta = lax.optimization_barrier(jnp.sum(g_block.astype(jnp.float32) * attn_out, axis=1, keepdims=True))
        grad_probs = contract_cols(g_block, value_rows)
        grad_scores = (attn_probs * (grad_probs - row_delta)).astype(jnp.bfloat16)
        q_grad = jnp.dot(grad_scores, k_bf, preferred_element_type=jnp.float32) * score_scale
        k_acc = k_acc + contract_rows(grad_scores, q_block) * score_scale
        v_acc = v_acc + contract_rows(probs_b, g_block)
        return ((k_acc, v_acc), q_grad)
    zeros_init = jnp.zeros(query_rows.shape, jnp.float32)
    (k_acc, v_acc), q_grads = lax.scan(one_block, (zeros_init, zeros_init), jnp.arange(length // block_rows, dtype=jnp.int32))
    grad_rq = q_grads.reshape(length, query_rows.shape[1])
    grad_q = q_back(grad_rq)[0].astype(jnp.bfloat16)
    grad_k = k_back(k_acc)[0].astype(jnp.bfloat16)
    return (grad_q, grad_k, v_acc.astype(jnp.bfloat16))

def reference(queries, keys, values, out_grad, layer_in, key_weight, value_weight, query_gain, key_gain):
    seq_count, length, _ = queries.shape
    group_size = HEADS // KV_HEADS

    def by_head(array):
        return array.reshape(seq_count, length, HEADS, HEAD_DIM).transpose(0, 2, 1, 3).reshape(seq_count * HEADS, length, HEAD_DIM)

    def widened(array):
        spread = jnp.broadcast_to(array.reshape(seq_count, length, KV_HEADS, 1, HEAD_DIM), (seq_count, length, KV_HEADS, group_size, HEAD_DIM))
        return by_head(spread.reshape(seq_count, length, HEADS * HEAD_DIM))

    def one_head(items):
        return head_grads(items[0], items[1], items[2], items[3], query_gain, key_gain)
    grad_q, grad_k, grad_v = lax.map(one_head, (by_head(queries), by_head(out_grad), widened(keys), widened(values)))
    grad_query = grad_q.reshape(seq_count, HEADS, length, HEAD_DIM).transpose(0, 2, 1, 3).reshape(seq_count, length, HEADS * HEAD_DIM)

    def grouped(array):
        summed = lax.optimization_barrier(jnp.sum(array.reshape(seq_count, KV_HEADS, group_size, length, HEAD_DIM).astype(jnp.float32), axis=2))
        return summed.astype(jnp.bfloat16).transpose(0, 2, 1, 3).reshape(seq_count * length, KV_HEADS * HEAD_DIM)
    kv_grad = jnp.concatenate([grouped(grad_k), grouped(grad_v)], axis=1)
    both_weights = jnp.concatenate([key_weight, value_weight], axis=1)
    grad_in = contract_cols(kv_grad, both_weights).astype(jnp.bfloat16).reshape(seq_count, length, layer_in.shape[2])
    weight_grad = contract_rows(layer_in.reshape(seq_count * length, layer_in.shape[2]), kv_grad)
    kv_width = KV_HEADS * HEAD_DIM
    return (grad_query, grad_in, weight_grad[:, :kv_width], weight_grad[:, kv_width:])
```

```python
import functools

import numpy as np
import jax
import jax.numpy as jnp
from jax import lax
from jax.experimental import pallas as pl
from jax.experimental.pallas import tpu as pltpu
from jax.sharding import PartitionSpec as P

HEAD_DIM = 128
GRID_W = 64
EPS = 1e-06
BASE = 10000.0
F32 = jnp.float32
BF16 = jnp.bfloat16


def dot(a, b, ca, cb):
    return lax.dot_general(a, b, (((ca,), (cb,)), ((), ())), preferred_element_type=F32)


def swapped(n):
    lane = lax.broadcasted_iota(jnp.int32, n.shape, 1)
    quarter = HEAD_DIM // 4
    return jnp.where(
        lane % (2 * quarter) < quarter,
        pltpu.roll(n, HEAD_DIM - quarter, 1),
        pltpu.roll(n, quarter, 1),
    )


def norm_rotate(u, gain, cosine, sine):
    r = lax.rsqrt(jnp.mean(u * u, axis=1, keepdims=True) + EPS)
    n = u * r * gain
    return n * cosine + swapped(n) * sine


def norm_rotate_back(u, gain, cosine, sine, grad):
    r = lax.rsqrt(jnp.mean(u * u, axis=1, keepdims=True) + EPS)
    dn = (grad * cosine - swapped(grad) * sine) * gain
    inner = jnp.mean(u * dn, axis=1, keepdims=True)
    return r * dn - u * (r * r * r * inner)


def tables(first, count):
    quarter = HEAD_DIM // 4
    inverse = (BASE ** (-np.arange(quarter) / quarter)).astype(np.float32)
    by_lane = jnp.asarray(np.tile(inverse, 4))[None, :]
    sign = jnp.asarray(np.tile(np.repeat([-1.0, 1.0], quarter), 2).astype(np.float32))[None, :]
    position = first + lax.broadcasted_iota(jnp.int32, (count, HEAD_DIM), 0)
    lane = lax.broadcasted_iota(jnp.int32, (count, HEAD_DIM), 1)
    where = jnp.where(lane < HEAD_DIM // 2, position // GRID_W, position % GRID_W)
    angle = where.astype(F32) * by_lane
    return jnp.cos(angle), jnp.sin(angle) * sign


def rotate_keys_kernel(kv_heads, k_ref, v_ref, gain_ref, cos_ref, sin_ref, out_ref):
    width = kv_heads * HEAD_DIM
    for h in range(kv_heads):
        cols = slice(h * HEAD_DIM, (h + 1) * HEAD_DIM)
        out_ref[:, cols] = norm_rotate(
            k_ref[:, cols].astype(F32), gain_ref[...], cos_ref[...], sin_ref[...]
        ).astype(BF16)
    out_ref[:, width:] = v_ref[...]


def attention_kernel(
    group, q_ref, g_ref, k_ref, v_ref, gain_ref, cos_ref, sin_ref, dq_ref, dkv_ref,
    rq, gs, pb, ds,
):
    rows = q_ref.shape[0]
    scale = HEAD_DIM ** (-0.5)
    k = k_ref[...]
    v = v_ref[...]
    for h in range(group):
        cols = slice(h * HEAD_DIM, (h + 1) * HEAD_DIM)
        here = slice(h * rows, (h + 1) * rows)
        rot = norm_rotate(
            q_ref[:, cols].astype(F32), gain_ref[...], cos_ref[...], sin_ref[...]
        ).astype(BF16)
        grad = g_ref[:, cols]
        rq[here, :] = rot
        gs[here, :] = grad
        scores = dot(rot, k, 1, 1) * scale
        e = jnp.exp(scores - jnp.max(scores, axis=1, keepdims=True))
        probs = e * (1.0 / jnp.sum(e, axis=1, keepdims=True))
        probs_b = probs.astype(BF16)
        out = dot(probs_b, v, 1, 0)
        delta = jnp.sum(grad.astype(F32) * out, axis=1, keepdims=True)
        gp = dot(grad, v, 1, 1)
        pb[here, :] = probs_b
        ds[here, :] = (probs * (gp - delta)).astype(BF16)
    dq = dot(ds[...], k, 1, 0) * scale
    for h in range(group):
        cols = slice(h * HEAD_DIM, (h + 1) * HEAD_DIM)
        dq_ref[:, cols] = norm_rotate_back(
            q_ref[:, cols].astype(F32), gain_ref[...], cos_ref[...], sin_ref[...],
            dq[h * rows : (h + 1) * rows, :],
        ).astype(BF16)
    dk = (dot(rq[...], ds[...], 0, 0) * scale).T.astype(BF16)
    dv = dot(gs[...], pb[...], 0, 0).T.astype(BF16)
    for s in range(dkv_ref.shape[0]):
        dkv_ref[s, 0] = dk[s * rows : (s + 1) * rows, :]
        dkv_ref[s, 1] = dv[s * rows : (s + 1) * rows, :]


def keys_back_kernel(kv_heads, k_ref, d_ref, gain_ref, cos_ref, sin_ref, out_ref):
    width = kv_heads * HEAD_DIM
    for h in range(kv_heads):
        cols = slice(h * HEAD_DIM, (h + 1) * HEAD_DIM)
        out_ref[:, cols] = norm_rotate_back(
            k_ref[:, cols].astype(F32), gain_ref[...], cos_ref[...], sin_ref[...],
            d_ref[0, :, cols].astype(F32),
        ).astype(BF16)
    out_ref[:, width:] = d_ref[1]


def on_device(
    n_sp, n_dp, queries, keys, values, out_grad, layer_in, key_weight, value_weight,
    query_gain, key_gain,
):
    _, rows, q_width = queries.shape
    kv_width = keys.shape[2]
    kv_heads = kv_width // HEAD_DIM
    group = q_width // kv_width
    length = rows * n_sp
    model = layer_in.shape[2]
    q_gain = query_gain[None, :]
    k_gain = key_gain[None, :]
    cosine, sine = tables(lax.axis_index("sp") * rows, rows)

    local = pl.pallas_call(
        functools.partial(rotate_keys_kernel, kv_heads),
        out_shape=jax.ShapeDtypeStruct((rows, 2 * kv_width), BF16),
    )(keys[0], values[0], k_gain, cosine, sine)
    gathered = lax.all_gather(local, "sp", axis=0, tiled=True)
    layer_cols = lax.all_to_all(
        layer_in.reshape(rows, n_dp, model // n_dp), "dp", split_axis=1, concat_axis=0, tiled=True
    ).reshape(n_dp * rows, model // n_dp)

    whole = lambda shape: pl.BlockSpec(shape, lambda i: (0,) * len(shape))
    wide = pl.BlockSpec((rows, group * HEAD_DIM), lambda i: (0, i))
    grad_query, partial = pl.pallas_call(
        functools.partial(attention_kernel, group),
        grid=(kv_heads,),
        in_specs=[
            wide,
            wide,
            pl.BlockSpec((length, HEAD_DIM), lambda i: (0, i)),
            pl.BlockSpec((length, HEAD_DIM), lambda i: (0, i + kv_heads)),
            whole((1, HEAD_DIM)),
            whole((rows, HEAD_DIM)),
            whole((rows, HEAD_DIM)),
        ],
        out_specs=[
            wide,
            pl.BlockSpec((n_sp, 2, rows, HEAD_DIM), lambda i: (0, 0, 0, i)),
        ],
        out_shape=[
            jax.ShapeDtypeStruct((rows, q_width), BF16),
            jax.ShapeDtypeStruct((n_sp, 2, rows, kv_width), BF16),
        ],
        scratch_shapes=[
            pltpu.VMEM((group * rows, HEAD_DIM), BF16),
            pltpu.VMEM((group * rows, HEAD_DIM), BF16),
            pltpu.VMEM((group * rows, length), BF16),
            pltpu.VMEM((group * rows, length), BF16),
        ],
        compiler_params=pltpu.CompilerParams(vmem_limit_bytes=48 * 2**20),
    )(queries[0], out_grad[0], gathered, gathered, q_gain, cosine, sine)

    summed = lax.psum_scatter(partial, "sp", scatter_dimension=0, tiled=True)
    kv_grad = pl.pallas_call(
        functools.partial(keys_back_kernel, kv_heads),
        out_shape=jax.ShapeDtypeStruct((rows, 2 * kv_width), BF16),
    )(keys[0], summed[0], k_gain, cosine, sine)

    kv_all = lax.all_gather(kv_grad, "dp", axis=0, tiled=True)
    part_in = (
        dot(kv_all[:, :kv_width], key_weight, 1, 1) + dot(kv_all[:, kv_width:], value_weight, 1, 1)
    ).astype(BF16)
    grad_in = lax.all_to_all(
        part_in.reshape(n_dp, rows, model // n_dp), "dp", split_axis=0, concat_axis=2, tiled=True
    )
    weight_grad = lax.psum(dot(layer_cols, kv_all, 0, 0).astype(BF16), "sp").astype(F32)
    return (
        grad_query[None],
        grad_in,
        weight_grad[:, :kv_width],
        weight_grad[:, kv_width:],
    )


def solution(mesh):
    tokens = P("dp", "sp", None)
    return jax.shard_map(
        functools.partial(on_device, mesh.shape["sp"], mesh.shape["dp"]),
        mesh=mesh,
        in_specs=(tokens,) * 5 + (P("dp", None), P("dp", None), P(), P()),
        out_specs=(tokens, tokens, P("dp", None), P("dp", None)),
        check_vma=False,
    )
```

```python
import functools
import math

import numpy as np
import jax
import jax.numpy as jnp
from jax import lax
from jax.experimental import pallas as pl
from jax.experimental.pallas import tpu as pltpu
from jax.sharding import PartitionSpec as P

HEAD_DIM = 128
GRID_W = 64
EPS = 1e-06
BASE = 10000.0
F32 = jnp.float32
BF16 = jnp.bfloat16


def dot(a, b, ca, cb):
    return lax.dot_general(a, b, (((ca,), (cb,)), ((), ())), preferred_element_type=F32)


def swapped(n):
    lane = lax.broadcasted_iota(jnp.int32, n.shape, 1)
    quarter = HEAD_DIM // 4
    return jnp.where(
        lane % (2 * quarter) < quarter,
        pltpu.roll(n, HEAD_DIM - quarter, 1),
        pltpu.roll(n, quarter, 1),
    )


def norm_rotate(u, gain, cosine, sine):
    r = lax.rsqrt(jnp.mean(u * u, axis=1, keepdims=True) + EPS)
    n = u * r * gain
    return n * cosine + swapped(n) * sine


def norm_rotate_back(u, gain, cosine, sine, grad):
    r = lax.rsqrt(jnp.mean(u * u, axis=1, keepdims=True) + EPS)
    dn = (grad * cosine - swapped(grad) * sine) * gain
    inner = jnp.mean(u * dn, axis=1, keepdims=True)
    return r * dn - u * (r * r * r * inner)


def tables(first, count):
    quarter = HEAD_DIM // 4
    inverse = (BASE ** (-np.arange(quarter) / quarter)).astype(np.float32)
    by_lane = jnp.asarray(np.tile(inverse, 4))[None, :]
    sign = jnp.asarray(np.tile(np.repeat([-1.0, 1.0], quarter), 2).astype(np.float32))[None, :]
    position = first + lax.broadcasted_iota(jnp.int32, (count, HEAD_DIM), 0)
    lane = lax.broadcasted_iota(jnp.int32, (count, HEAD_DIM), 1)
    where = jnp.where(lane < HEAD_DIM // 2, position // GRID_W, position % GRID_W)
    angle = where.astype(F32) * by_lane
    return jnp.cos(angle), jnp.sin(angle) * sign


def ring_order(n):
    across = 2 ** ((n.bit_length() - 1) // 2)
    down = n // across
    cells = [(z, 0) for z in range(down)]
    for z in reversed(range(down)):
        line = [(z, x) for x in range(1, across)]
        cells += line if (down - 1 - z) % 2 == 0 else line[::-1]
    return [z * across + x for z, x in cells]


def pick(table, index):
    return sum(jnp.where(index == i, jnp.int32(v), 0) for i, v in enumerate(table))


def rows_of(c, d, size):
    half = size // 2
    return pl.ds(pl.multiple_of(c * size + d * half, half), half)


def ring_gather(buf, size, n, pos, sides, send, recv, hook=None):
    copies = []
    for s in range(n - 1):
        for d in range(2):
            c = lax.rem(pos + n - s, n) if d == 0 else lax.rem(pos + s, n)
            if s > 0:
                copies[2 * (s - 1) + d].wait_recv()
            part = buf.at[rows_of(c, d, size)]
            copy = pltpu.make_async_remote_copy(
                part, part, send.at[d, s], recv.at[d, s], device_id={"sp": sides[d]}
            )
            copy.start()
            copies.append(copy)
        if s == 0 and hook is not None:
            hook()
    for d in range(2):
        copies[2 * (n - 2) + d].wait_recv()
    for copy in copies:
        copy.wait_send()


def ring_scatter(own, slots, size, n, pos, sides, send, recv, finish, hook=None):
    copies = []
    half = size // 2
    for s in range(n):
        for d in range(2):
            c = lax.rem(pos + 2 * n - s - 1, n) if d == 0 else lax.rem(pos + s + 1, n)
            source = own.at[rows_of(c, d, size)]
            if s > 0:
                copies[2 * (s - 1) + d].wait_recv()
                slot = slots.at[pl.ds((s - 1) * size + d * half, half)]
                total = slot[...].astype(F32) + source[...].astype(F32)
                if s == n - 1:
                    finish(d, total)
                    continue
                slot[...] = total.astype(BF16)
                source = slot
            copy = pltpu.make_async_remote_copy(
                source, slots.at[pl.ds(s * size + d * half, half)],
                send.at[d, s], recv.at[d, s], device_id={"sp": sides[d]},
            )
            copy.start()
            copies.append(copy)
        if s == 0 and hook is not None:
            hook()
    for copy in copies:
        copy.wait_send()


def fused_kernel(
    n_sp, n_dp, q_ref, k_ref, v_ref, g_ref, layer_ref, wk_ref, wv_ref, qg_ref, kg_ref,
    cos_ref, sin_ref, dq_ref, din_ref, gw_ref,
    kv, part, slots, rq, gs, pb, ds, back, lc, kvall, gin, gwpart, gwslots,
    ag_s, ag_r, rs_s, rs_r, ws_s, ws_r, wa_s, wa_r, lx_s, lx_r, kx_s, kx_r, gx_s, gx_r,
):
    rows, q_width = q_ref.shape
    kv_width = k_ref.shape[1]
    kv_heads = kv_width // HEAD_DIM
    group = q_width // kv_width
    length = rows * n_sp
    wide = wk_ref.shape[0]
    share = wide // n_sp
    scale = HEAD_DIM ** (-0.5)
    me = lax.axis_index("sp")
    mine = lax.axis_index("dp")
    order = ring_order(n_sp)
    place = [order.index(i) for i in range(n_sp)]
    pos = pick(place, me)
    sides = (
        pick([order[(place[i] + 1) % n_sp] for i in range(n_sp)], me),
        pick([order[(place[i] - 1) % n_sp] for i in range(n_sp)], me),
    )
    peers = [lax.rem(mine + j, n_dp) for j in range(1, n_dp)]

    barrier = pltpu.get_barrier_semaphore()
    for side in sides:
        pl.semaphore_signal(barrier, inc=1, device_id={"sp": side})
    for peer in peers:
        pl.semaphore_signal(barrier, inc=1, device_id={"dp": peer})
    pl.semaphore_wait(barrier, 2 + len(peers))

    own_rows = pl.ds(pl.multiple_of(pos * rows, rows), rows)
    for h in range(kv_heads):
        cols = slice(h * HEAD_DIM, (h + 1) * HEAD_DIM)
        kv[own_rows, cols] = norm_rotate(
            k_ref[:, cols].astype(F32), kg_ref[...], cos_ref[...], sin_ref[...]
        ).astype(BF16)
    kv[own_rows, kv_width:] = v_ref[...]

    def dcols(j):
        return pl.ds(pl.multiple_of(j * wide, wide), wide)

    def drows(j):
        return pl.ds(pl.multiple_of(j * rows, rows), rows)

    exchange = []

    def start_exchange():
        for j, peer in enumerate(peers):
            copy = pltpu.make_async_remote_copy(
                layer_ref.at[:, dcols(peer)], lc.at[drows(mine)], lx_s.at[j], lx_r.at[j],
                device_id={"dp": peer},
            )
            copy.start()
            exchange.append(copy)
        lc[drows(mine), :] = layer_ref[:, dcols(mine)]

    ring_gather(kv, rows, n_sp, pos, sides, ag_s, ag_r, start_exchange)

    def one_head(i, carry):
        kcols = pl.ds(pl.multiple_of(i * HEAD_DIM, HEAD_DIM), HEAD_DIM)
        vcols = pl.ds(pl.multiple_of(kv_width + i * HEAD_DIM, HEAD_DIM), HEAD_DIM)
        k = kv[:, kcols]
        v = kv[:, vcols]

        def qcols(h):
            return pl.ds(pl.multiple_of((i * group + h) * HEAD_DIM, HEAD_DIM), HEAD_DIM)

        for h in range(group):
            here = slice(h * rows, (h + 1) * rows)
            rot = norm_rotate(
                q_ref[:, qcols(h)].astype(F32), qg_ref[...], cos_ref[...], sin_ref[...]
            ).astype(BF16)
            grad = g_ref[:, qcols(h)]
            rq[here, :] = rot
            gs[here, :] = grad
            scores = dot(rot, k, 1, 1) * scale
            e = jnp.exp(scores - jnp.max(scores, axis=1, keepdims=True))
            probs = e * (1.0 / jnp.sum(e, axis=1, keepdims=True))
            probs_b = probs.astype(BF16)
            out = dot(probs_b, v, 1, 0)
            delta = jnp.sum(grad.astype(F32) * out, axis=1, keepdims=True)
            gp = dot(grad, v, 1, 1)
            pb[here, :] = probs_b
            ds[here, :] = (probs * (gp - delta)).astype(BF16)
        dq = dot(ds[...], k, 1, 0) * scale
        for h in range(group):
            dq_ref[:, qcols(h)] = norm_rotate_back(
                q_ref[:, qcols(h)].astype(F32), qg_ref[...], cos_ref[...], sin_ref[...],
                dq[h * rows : (h + 1) * rows, :],
            ).astype(BF16)
        part[:, kcols] = (dot(rq[...], ds[...], 0, 0) * scale).T.astype(BF16)
        part[:, vcols] = dot(gs[...], pb[...], 0, 0).T.astype(BF16)
        return carry

    lax.fori_loop(0, kv_heads, one_head, 0)

    def keep_back(d, total):
        back[d * (rows // 2) : (d + 1) * (rows // 2), :] = total

    ring_scatter(part, slots, rows, n_sp, pos, sides, rs_s, rs_r, keep_back)

    for h in range(kv_heads):
        cols = slice(h * HEAD_DIM, (h + 1) * HEAD_DIM)
        kvall[drows(mine), cols] = norm_rotate_back(
            k_ref[:, cols].astype(F32), kg_ref[...], cos_ref[...], sin_ref[...], back[:, cols]
        ).astype(BF16)
    kvall[drows(mine), kv_width:] = back[:, kv_width:].astype(BF16)
    spread = []
    for j, peer in enumerate(peers):
        copy = pltpu.make_async_remote_copy(
            kvall.at[drows(mine)], kvall.at[drows(mine)], kx_s.at[j], kx_r.at[j],
            device_id={"dp": peer},
        )
        copy.start()
        spread.append(copy)
    for copy in exchange:
        copy.wait()
    for copy in spread:
        copy.wait()

    block = math.gcd(wide, HEAD_DIM)

    for b in range(wide // block):
        cols = slice(b * block, (b + 1) * block)
        gwpart[cols, :] = dot(lc[:, cols], kvall[...], 0, 0).astype(BF16)

    returned = []

    def inputs_part(j):
        return (
            dot(kvall[drows(j), :kv_width], wk_ref[...], 1, 1)
            + dot(kvall[drows(j), kv_width:], wv_ref[...], 1, 1)
        ).astype(BF16)

    def send_inputs():
        for j, peer in enumerate(peers):
            gin[j] = inputs_part(peer)
            copy = pltpu.make_async_remote_copy(
                gin.at[j], din_ref.at[:, dcols(mine)], gx_s.at[j], gx_r.at[j],
                device_id={"dp": peer},
            )
            copy.start()
            returned.append(copy)
        din_ref[:, dcols(mine)] = inputs_part(mine)

    def keep_weight(d, total):
        gw_ref[rows_of(pos, d, share), :] = total.astype(BF16)

    ring_scatter(
        gwpart, gwslots, share, n_sp, pos, sides, ws_s, ws_r, keep_weight, send_inputs
    )
    ring_gather(gw_ref, share, n_sp, pos, sides, wa_s, wa_r)
    for copy in returned:
        copy.wait()


def on_device(
    n_sp, n_dp, queries, keys, values, out_grad, layer_in, key_weight, value_weight,
    query_gain, key_gain,
):
    _, rows, q_width = queries.shape
    kv_width = keys.shape[2]
    group = q_width // kv_width
    length = rows * n_sp
    model = layer_in.shape[2]
    wide = model // n_dp
    both = 2 * kv_width
    cosine, sine = tables(lax.axis_index("sp") * rows, rows)
    ring = pltpu.SemaphoreType.DMA((2, n_sp - 1))
    direct = pltpu.SemaphoreType.DMA((n_dp - 1,))
    vmem = pl.BlockSpec(memory_space=pltpu.VMEM)
    grad_query, grad_in, weight_grad = pl.pallas_call(
        functools.partial(fused_kernel, n_sp, n_dp),
        in_specs=[vmem] * 11,
        out_specs=[vmem] * 3,
        out_shape=[
            jax.ShapeDtypeStruct((rows, q_width), BF16),
            jax.ShapeDtypeStruct((rows, model), BF16),
            jax.ShapeDtypeStruct((wide, both), BF16),
        ],
        scratch_shapes=[
            pltpu.VMEM((length, both), BF16),
            pltpu.VMEM((length, both), BF16),
            pltpu.VMEM(((n_sp - 1) * rows, both), BF16),
            pltpu.VMEM((group * rows, HEAD_DIM), BF16),
            pltpu.VMEM((group * rows, HEAD_DIM), BF16),
            pltpu.VMEM((group * rows, length), BF16),
            pltpu.VMEM((group * rows, length), BF16),
            pltpu.VMEM((rows, both), F32),
            pltpu.VMEM((n_dp * rows, wide), BF16),
            pltpu.VMEM((n_dp * rows, both), BF16),
            pltpu.VMEM((n_dp - 1, rows, wide), BF16),
            pltpu.VMEM((wide, both), BF16),
            pltpu.VMEM((wide * (n_sp - 1) // n_sp, both), BF16),
        ] + [ring] * 8 + [direct] * 6,
        compiler_params=pltpu.CompilerParams(
            collective_id=0, has_side_effects=True, vmem_limit_bytes=58 * 2**20
        ),
    )(
        queries[0], keys[0], values[0], out_grad[0], layer_in[0], key_weight, value_weight,
        query_gain[None, :], key_gain[None, :], cosine, sine,
    )
    weight_grad = weight_grad.astype(F32)
    return (
        grad_query[None],
        grad_in[None],
        weight_grad[:, :kv_width],
        weight_grad[:, kv_width:],
    )


def solution(mesh):
    tokens = P("dp", "sp", None)
    return jax.shard_map(
        functools.partial(on_device, mesh.shape["sp"], mesh.shape["dp"]),
        mesh=mesh,
        in_specs=(tokens,) * 5 + (P("dp", None), P("dp", None), P(), P()),
        out_specs=(tokens, tokens, P("dp", None), P("dp", None)),
        check_vma=False,
    )
```

```python
import functools
import math

import numpy as np
import jax
import jax.numpy as jnp
from jax import lax
from jax.experimental import pallas as pl
from jax.experimental.pallas import tpu as pltpu
from jax.sharding import PartitionSpec as P

HEAD_DIM = 128
GRID_W = 64
EPS = 1e-06
BASE = 10000.0
PIECES = 4
F32 = jnp.float32
BF16 = jnp.bfloat16


def dot(a, b, ca, cb):
    return lax.dot_general(a, b, (((ca,), (cb,)), ((), ())), preferred_element_type=F32)


def swapped(n):
    lane = lax.broadcasted_iota(jnp.int32, n.shape, 1)
    quarter = HEAD_DIM // 4
    return jnp.where(
        lane % (2 * quarter) < quarter,
        pltpu.roll(n, HEAD_DIM - quarter, 1),
        pltpu.roll(n, quarter, 1),
    )


def norm_rotate(u, gain, cosine, sine):
    r = lax.rsqrt(jnp.mean(u * u, axis=1, keepdims=True) + EPS)
    n = u * r * gain
    return n * cosine + swapped(n) * sine


def norm_rotate_back(u, gain, cosine, sine, grad):
    r = lax.rsqrt(jnp.mean(u * u, axis=1, keepdims=True) + EPS)
    dn = (grad * cosine - swapped(grad) * sine) * gain
    inner = jnp.mean(u * dn, axis=1, keepdims=True)
    return r * dn - u * (r * r * r * inner)


def tables(first, count):
    quarter = HEAD_DIM // 4
    inverse = (BASE ** (-np.arange(quarter) / quarter)).astype(np.float32)
    by_lane = jnp.asarray(np.tile(inverse, 4))[None, :]
    sign = jnp.asarray(np.tile(np.repeat([-1.0, 1.0], quarter), 2).astype(np.float32))[None, :]
    position = first + lax.broadcasted_iota(jnp.int32, (count, HEAD_DIM), 0)
    lane = lax.broadcasted_iota(jnp.int32, (count, HEAD_DIM), 1)
    where = jnp.where(lane < HEAD_DIM // 2, position // GRID_W, position % GRID_W)
    angle = where.astype(F32) * by_lane
    return jnp.cos(angle), jnp.sin(angle) * sign


def ring_order(n):
    across = 2 ** ((n.bit_length() - 1) // 2)
    down = n // across
    cells = [(z, 0) for z in range(down)]
    for z in reversed(range(down)):
        line = [(z, x) for x in range(1, across)]
        cells += line if (down - 1 - z) % 2 == 0 else line[::-1]
    return [z * across + x for z, x in cells]


def pick(table, index):
    return sum(jnp.where(index == i, jnp.int32(v), 0) for i, v in enumerate(table))


def rows_of(c, d, size):
    half = size // 2
    return pl.ds(pl.multiple_of(c * size + d * half, half), half)


def lanes_of(ref, q):
    width = ref.shape[1] // PIECES
    return pl.ds(q * width, width)


def ring_gather(buf, size, n, pos, sides, send, recv, hook=None):
    copies = {}
    streams = [(d, q) for q in range(PIECES) for d in range(2)]
    for s in range(n - 1):
        for d, q in streams:
            c = lax.rem(pos + n - s, n) if d == 0 else lax.rem(pos + s, n)
            if s > 0:
                copies[s - 1, d, q].wait_recv()
            part = buf.at[rows_of(c, d, size), lanes_of(buf, q)]
            copies[s, d, q] = pltpu.make_async_remote_copy(
                part, part, send.at[d * PIECES + q, s], recv.at[d * PIECES + q, s],
                device_id={"sp": sides[d]},
            )
            copies[s, d, q].start()
        if s == 0 and hook is not None:
            hook()
    for d, q in streams:
        copies[n - 2, d, q].wait_recv()
    for copy in copies.values():
        copy.wait_send()


def ring_scatter(own, slots, size, n, pos, sides, send, recv, finish, hook=None):
    copies = {}
    half = size // 2
    streams = [(d, q) for q in range(PIECES) for d in range(2)]
    for s in range(n):
        for d, q in streams:
            c = lax.rem(pos + 2 * n - s - 1, n) if d == 0 else lax.rem(pos + s + 1, n)
            cols = lanes_of(own, q)
            source = own.at[rows_of(c, d, size), cols]
            if s > 0:
                copies[s - 1, d, q].wait_recv()
                slot = slots.at[pl.ds((s - 1) * size + d * half, half), cols]
                total = slot[...].astype(F32) + source[...].astype(F32)
                if s == n - 1:
                    finish(d, cols, total)
                    continue
                slot[...] = total.astype(BF16)
                source = slot
            copies[s, d, q] = pltpu.make_async_remote_copy(
                source, slots.at[pl.ds(s * size + d * half, half), cols],
                send.at[d * PIECES + q, s], recv.at[d * PIECES + q, s],
                device_id={"sp": sides[d]},
            )
            copies[s, d, q].start()
        if s == 0 and hook is not None:
            hook()
    for copy in copies.values():
        copy.wait_send()


def fused_kernel(
    n_sp, n_dp, q_ref, k_ref, v_ref, g_ref, layer_ref, wk_ref, wv_ref, qg_ref, kg_ref,
    cos_ref, sin_ref, dq_ref, din_ref, gw_ref,
    kv, part, slots, rq, gs, pb, ds, back, lc, kvall, gin, gwpart, gwslots,
    ag_s, ag_r, rs_s, rs_r, ws_s, ws_r, wa_s, wa_r, lx_s, lx_r, kx_s, kx_r, gx_s, gx_r,
):
    rows, q_width = q_ref.shape
    kv_width = k_ref.shape[1]
    kv_heads = kv_width // HEAD_DIM
    group = q_width // kv_width
    length = rows * n_sp
    wide = wk_ref.shape[0]
    share = wide // n_sp
    scale = HEAD_DIM ** (-0.5)
    me = lax.axis_index("sp")
    mine = lax.axis_index("dp")
    order = ring_order(n_sp)
    place = [order.index(i) for i in range(n_sp)]
    pos = pick(place, me)
    sides = (
        pick([order[(place[i] + 1) % n_sp] for i in range(n_sp)], me),
        pick([order[(place[i] - 1) % n_sp] for i in range(n_sp)], me),
    )
    peers = [lax.rem(mine + j, n_dp) for j in range(1, n_dp)]

    barrier = pltpu.get_barrier_semaphore()
    for side in sides:
        pl.semaphore_signal(barrier, inc=1, device_id={"sp": side})
    for peer in peers:
        pl.semaphore_signal(barrier, inc=1, device_id={"dp": peer})
    pl.semaphore_wait(barrier, 2 + len(peers))

    own_rows = pl.ds(pl.multiple_of(pos * rows, rows), rows)
    for h in range(kv_heads):
        cols = slice(h * HEAD_DIM, (h + 1) * HEAD_DIM)
        kv[own_rows, cols] = norm_rotate(
            k_ref[:, cols].astype(F32), kg_ref[...], cos_ref[...], sin_ref[...]
        ).astype(BF16)
    kv[own_rows, kv_width:] = v_ref[...]

    def dcols(j):
        return pl.ds(pl.multiple_of(j * wide, wide), wide)

    def drows(j):
        return pl.ds(pl.multiple_of(j * rows, rows), rows)

    exchange = []

    def start_exchange():
        for j, peer in enumerate(peers):
            copy = pltpu.make_async_remote_copy(
                layer_ref.at[:, dcols(peer)], lc.at[drows(mine)], lx_s.at[j], lx_r.at[j],
                device_id={"dp": peer},
            )
            copy.start()
            exchange.append(copy)
        lc[drows(mine), :] = layer_ref[:, dcols(mine)]

    ring_gather(kv, rows, n_sp, pos, sides, ag_s, ag_r, start_exchange)

    def one_head(i, carry):
        kcols = pl.ds(pl.multiple_of(i * HEAD_DIM, HEAD_DIM), HEAD_DIM)
        vcols = pl.ds(pl.multiple_of(kv_width + i * HEAD_DIM, HEAD_DIM), HEAD_DIM)
        k = kv[:, kcols]
        v = kv[:, vcols]

        def qcols(h):
            return pl.ds(pl.multiple_of((i * group + h) * HEAD_DIM, HEAD_DIM), HEAD_DIM)

        for h in range(group):
            here = slice(h * rows, (h + 1) * rows)
            rot = norm_rotate(
                q_ref[:, qcols(h)].astype(F32), qg_ref[...], cos_ref[...], sin_ref[...]
            ).astype(BF16)
            grad = g_ref[:, qcols(h)]
            rq[here, :] = rot
            gs[here, :] = grad
            scores = dot(rot, k, 1, 1) * scale
            e = jnp.exp(scores - jnp.max(scores, axis=1, keepdims=True))
            probs = e * (1.0 / jnp.sum(e, axis=1, keepdims=True))
            probs_b = probs.astype(BF16)
            out = dot(probs_b, v, 1, 0)
            delta = jnp.sum(grad.astype(F32) * out, axis=1, keepdims=True)
            gp = dot(grad, v, 1, 1)
            pb[here, :] = probs_b
            ds[here, :] = (probs * (gp - delta)).astype(BF16)
        dq = dot(ds[...], k, 1, 0) * scale
        for h in range(group):
            dq_ref[:, qcols(h)] = norm_rotate_back(
                q_ref[:, qcols(h)].astype(F32), qg_ref[...], cos_ref[...], sin_ref[...],
                dq[h * rows : (h + 1) * rows, :],
            ).astype(BF16)
        part[:, kcols] = (dot(rq[...], ds[...], 0, 0) * scale).T.astype(BF16)
        part[:, vcols] = dot(gs[...], pb[...], 0, 0).T.astype(BF16)
        return carry

    lax.fori_loop(0, kv_heads, one_head, 0)

    def keep_back(d, cols, total):
        back[d * (rows // 2) : (d + 1) * (rows // 2), cols] = total

    ring_scatter(part, slots, rows, n_sp, pos, sides, rs_s, rs_r, keep_back)

    for h in range(kv_heads):
        cols = slice(h * HEAD_DIM, (h + 1) * HEAD_DIM)
        kvall[drows(mine), cols] = norm_rotate_back(
            k_ref[:, cols].astype(F32), kg_ref[...], cos_ref[...], sin_ref[...], back[:, cols]
        ).astype(BF16)
    kvall[drows(mine), kv_width:] = back[:, kv_width:].astype(BF16)
    spread = []
    for j, peer in enumerate(peers):
        copy = pltpu.make_async_remote_copy(
            kvall.at[drows(mine)], kvall.at[drows(mine)], kx_s.at[j], kx_r.at[j],
            device_id={"dp": peer},
        )
        copy.start()
        spread.append(copy)
    for copy in exchange:
        copy.wait()
    for copy in spread:
        copy.wait()

    block = math.gcd(wide, HEAD_DIM)

    for b in range(wide // block):
        cols = slice(b * block, (b + 1) * block)
        gwpart[cols, :] = dot(lc[:, cols], kvall[...], 0, 0).astype(BF16)

    returned = []

    def inputs_part(j):
        return (
            dot(kvall[drows(j), :kv_width], wk_ref[...], 1, 1)
            + dot(kvall[drows(j), kv_width:], wv_ref[...], 1, 1)
        ).astype(BF16)

    def send_inputs():
        for j, peer in enumerate(peers):
            gin[j] = inputs_part(peer)
            copy = pltpu.make_async_remote_copy(
                gin.at[j], din_ref.at[:, dcols(mine)], gx_s.at[j], gx_r.at[j],
                device_id={"dp": peer},
            )
            copy.start()
            returned.append(copy)
        din_ref[:, dcols(mine)] = inputs_part(mine)

    def keep_weight(d, cols, total):
        gw_ref[rows_of(pos, d, share), cols] = total.astype(BF16)

    ring_scatter(
        gwpart, gwslots, share, n_sp, pos, sides, ws_s, ws_r, keep_weight, send_inputs
    )
    ring_gather(gw_ref, share, n_sp, pos, sides, wa_s, wa_r)
    for copy in returned:
        copy.wait()


def on_device(
    n_sp, n_dp, queries, keys, values, out_grad, layer_in, key_weight, value_weight,
    query_gain, key_gain,
):
    _, rows, q_width = queries.shape
    kv_width = keys.shape[2]
    group = q_width // kv_width
    length = rows * n_sp
    model = layer_in.shape[2]
    wide = model // n_dp
    both = 2 * kv_width
    cosine, sine = tables(lax.axis_index("sp") * rows, rows)
    ring = pltpu.SemaphoreType.DMA((2 * PIECES, n_sp - 1))
    direct = pltpu.SemaphoreType.DMA((n_dp - 1,))
    vmem = pl.BlockSpec(memory_space=pltpu.VMEM)
    grad_query, grad_in, weight_grad = pl.pallas_call(
        functools.partial(fused_kernel, n_sp, n_dp),
        in_specs=[vmem] * 11,
        out_specs=[vmem] * 3,
        out_shape=[
            jax.ShapeDtypeStruct((rows, q_width), BF16),
            jax.ShapeDtypeStruct((rows, model), BF16),
            jax.ShapeDtypeStruct((wide, both), BF16),
        ],
        scratch_shapes=[
            pltpu.VMEM((length, both), BF16),
            pltpu.VMEM((length, both), BF16),
            pltpu.VMEM(((n_sp - 1) * rows, both), BF16),
            pltpu.VMEM((group * rows, HEAD_DIM), BF16),
            pltpu.VMEM((group * rows, HEAD_DIM), BF16),
            pltpu.VMEM((group * rows, length), BF16),
            pltpu.VMEM((group * rows, length), BF16),
            pltpu.VMEM((rows, both), F32),
            pltpu.VMEM((n_dp * rows, wide), BF16),
            pltpu.VMEM((n_dp * rows, both), BF16),
            pltpu.VMEM((n_dp - 1, rows, wide), BF16),
            pltpu.VMEM((wide, both), BF16),
            pltpu.VMEM((wide * (n_sp - 1) // n_sp, both), BF16),
        ] + [ring] * 8 + [direct] * 6,
        compiler_params=pltpu.CompilerParams(
            collective_id=0, has_side_effects=True, vmem_limit_bytes=58 * 2**20
        ),
    )(
        queries[0], keys[0], values[0], out_grad[0], layer_in[0], key_weight, value_weight,
        query_gain[None, :], key_gain[None, :], cosine, sine,
    )
    weight_grad = weight_grad.astype(F32)
    return (
        grad_query[None],
        grad_in[None],
        weight_grad[:, :kv_width],
        weight_grad[:, kv_width:],
    )


def solution(mesh):
    tokens = P("dp", "sp", None)
    return jax.shard_map(
        functools.partial(on_device, mesh.shape["sp"], mesh.shape["dp"]),
        mesh=mesh,
        in_specs=(tokens,) * 5 + (P("dp", None), P("dp", None), P(), P()),
        out_specs=(tokens, tokens, P("dp", None), P("dp", None)),
        check_vma=False,
    )
```
